32 devices in a mesh: ep: 8 (over z, x), tp: 4 (over y, core).
Axes of the slice: x: 2, y: 2, z: 4, core: 2. Of those that a mesh axis runs over, the one named last changes fastest.
Arguments:
- hidden: bfloat16 [256, 4096], P('ep', 'tp'), may hold values from -6 to 6
- norm_gain: float32 [4096], P('tp'), may hold values from 0.1 to 1.9
- expert_ids: int32 [256, 8], P('ep'), may hold values from 0 to 15, as said below
- route_weights: float32 [256, 8], P('ep'), may hold values from 0.1 to 1
- lengths: int32 [32], P('ep'), may hold values from 1 to 8, as said below
- gate_proj: bfloat16 [16, 4096, 1024], P('ep', None, 'tp'), may hold values from -0.09375 to 0.09375
- up_proj: bfloat16 [16, 4096, 1024], P('ep', None, 'tp'), may hold values from -0.09375 to 0.09375
- down_proj: bfloat16 [16, 1024, 4096], P('ep', 'tp'), may hold values from -0.1875 to 0.1875
- shared_gate: bfloat16 [4096, 1024], P(None, 'tp'), may hold values from -0.09375 to 0.09375
- shared_up: bfloat16 [4096, 1024], P(None, 'tp'), may hold values from -0.09375 to 0.09375
- shared_down: bfloat16 [1024, 4096], P('tp'), may hold values from -0.1875 to 0.1875
Outputs:
- mixed: bfloat16 [256, 4096], P('ep', 'tp')
The draws below stay inside these ranges and needn't reach their ends.
Inputs may be any that keep to these rules, and one draw needn't show every extreme that they name: `expert_ids`: among the 32 rows of one index of ep (an aligned block), no expert is named more than 32 times, and in every block one expert is named exactly 32 times; each row names 8 different experts. `lengths`: each sequence has 1 to 8 live slots; on some index of ep all 4 sequences have 8 live slots.
All inputs are finite; a program needn't handle non-finite values.
Results may differ from the reference program's by a relative error of at most 0.015.
Values may be sent and summed in bfloat16 or wider, within the bound.
A program may use at most 128 MiB of HBM per device.

```python
import jax
import jax.numpy as jnp
import numpy as np
from jax import lax

D = 4096
FF = 1024
SFF = 1024
TOP = 8
SPAN = 8
SEQ_DEV = 4
EXPERTS = 16
SEQS = 32
SLOTS_DEV = 32
ROWS = 256
CAP = 32
N_EP = 8


def rank_counts():
    others = EXPERTS - 1
    tier_weights = []
    for rank in range(others):
        if rank < others // 8:
            tier_weights.append(3)
        elif rank < others // 2:
            tier_weights.append(2)
        else:
            tier_weights.append(1)
    leftover = SLOTS_DEV * TOP - CAP
    counts = [0] * others
    height = 0
    while leftover > 0:
        height = height + 1
        for rank in range(others):
            if leftover > 0:
                target = min(CAP, tier_weights[rank] * height)
                added = min(max(target - counts[rank], 0), leftover)
                counts[rank] = counts[rank] + added
                leftover = leftover - added
    return [CAP] + counts


def one_block(block_key, rank_table):
    order_key, row_key, column_key = jax.random.split(block_key, 3)
    label_order = jax.random.permutation(order_key, EXPERTS).astype(jnp.int32)
    labels = label_order[rank_table]
    chosen = labels.reshape(TOP, SLOTS_DEV).T
    row_order = jax.random.permutation(row_key, SLOTS_DEV)
    chosen = chosen[row_order]
    scores = jax.random.randint(column_key, (SLOTS_DEV, TOP), 0, 1 << 20) * TOP + jnp.arange(TOP, dtype=jnp.int32)[None, :]
    column_order = jnp.argsort(scores, axis=1, stable=True)
    return jnp.take_along_axis(chosen, column_order, axis=1).astype(jnp.int32)


def draw_expert_ids(key, part):
    block_count = SEQS // SEQ_DEV
    rank_table = jnp.asarray(np.repeat(np.arange(EXPERTS), np.array(rank_counts())), dtype=jnp.int32)
    block_keys = jax.random.split(jax.random.fold_in(key, 11), block_count)
    blocks = jax.vmap(lambda single_key: one_block(single_key, rank_table))(block_keys)
    return blocks.reshape(block_count * SLOTS_DEV, TOP).astype(jnp.int32)


def draw_lengths(key, part):
    short_key, long_key, pick_key, block_key = jax.random.split(jax.random.fold_in(key, 23), 4)
    short_len = jax.random.randint(short_key, (SEQS,), 1, 3)
    long_len = jax.random.randint(long_key, (SEQS,), SPAN // 2 + 1, SPAN + 1)
    picked = jax.random.randint(pick_key, (SEQS,), 0, 4) == 0
    drawn = jnp.where(picked, long_len, short_len)
    full_block = jax.random.randint(block_key, (), 0, SEQS // SEQ_DEV)
    owner = jnp.arange(SEQS, dtype=jnp.int32) // SEQ_DEV
    return jnp.where(owner == full_block, SPAN, drawn).astype(jnp.int32)


def level_of(own_key, extent, shards, low, top_value):
    def one(dim, blocks):
        heights = jax.random.uniform(jax.random.fold_in(jax.random.fold_in(own_key, 6), dim), (blocks,), jnp.float32, low / len(shards), top_value / len(shards))
        return jnp.repeat(jnp.exp(heights), extent[dim] // blocks).reshape((-1,) + (1,) * (len(extent) - dim - 1))

    gain = one(*shards[0])
    for cut in shards[1:]:
        gain = gain * one(*cut)
    return gain


def noise(key, shape, spread, bound, cuts=(), held_as=jnp.bfloat16):
    gain = level_of(key, shape, cuts, -0.22, 0.18) if cuts else 1.0
    entries = jax.random.normal(key, shape, jnp.float32) * spread * gain
    return jnp.minimum(jnp.maximum(entries, -bound), bound).astype(held_as)


def setup_inputs(seed: int = 0) -> dict:
    splits = jax.random.split(jax.random.key(seed), 12)
    return {
        "hidden": noise(splits[0], (ROWS, D), 1.0, 6.0, ((0, 8), (1, 4))),
        "norm_gain": jnp.clip(1.0 + 0.18 * jax.random.normal(splits[1], (D,), jnp.float32), 0.1, 1.9),
        "expert_ids": draw_expert_ids(jax.random.fold_in(splits[11], 71), 0),
        "route_weights": jnp.clip(0.1 + 0.9 * jax.random.uniform(splits[3], (ROWS, TOP), jnp.float32) ** level_of(splits[3], (ROWS, TOP), ((0, 8),), -0.2, 0.2), 0.1, 1.0),
        "lengths": draw_lengths(jax.random.fold_in(splits[11], 71), 0),
        "gate_proj": noise(splits[5], (EXPERTS, D, FF), D ** -0.5, 0.09375, ((0, 8), (2, 4))),
        "up_proj": noise(splits[6], (EXPERTS, D, FF), D ** -0.5, 0.09375, ((0, 8), (2, 4))),
        "down_proj": noise(splits[7], (EXPERTS, FF, D), FF ** -0.5, 0.1875, ((0, 8), (1, 4))),
        "shared_gate": noise(splits[8], (D, SFF), D ** -0.5, 0.09375, ((1, 4),)),
        "shared_up": noise(splits[9], (D, SFF), D ** -0.5, 0.09375, ((1, 4),)),
        "shared_down": noise(splits[10], (SFF, D), SFF ** -0.5, 0.1875, ((0, 4),)),
    }


epsilon = 1e-06

def reference(hidden, norm_gain, expert_ids, route_weights, lengths, gate_proj, up_proj, down_proj, shared_gate, shared_up, shared_down):
    row_count = hidden.shape[0]
    values = hidden.astype(jnp.float32)
    normed = (values * lax.rsqrt(lax.optimization_barrier(jnp.mean(values * values, axis=1, keepdims=True)) + epsilon) * norm_gain[None, :]).astype(jnp.bfloat16)
    offsets = jnp.arange(row_count, dtype=jnp.int32) % SPAN
    is_live = offsets < jnp.repeat(lengths, SPAN)
    mixing = jnp.where(is_live[:, None], route_weights, 0.0)
    expert_range = jnp.arange(EXPERTS, dtype=jnp.int32)
    is_named = (expert_ids[:, :, None] == expert_range[None, None, :]) & is_live[:, None, None]
    by_expert = lax.optimization_barrier(jnp.sum(jnp.where(is_named, mixing[:, :, None], 0.0), axis=1))
    hit_any = jnp.any(is_named, axis=1)
    row_order = (row_count - jnp.arange(row_count, dtype=jnp.int32)).astype(jnp.int32)
    pick_count = min(row_count, N_EP * CAP)

    def one_expert(accumulated, per_expert):
        hit_column, mix_column, w_gate, w_up, w_down = per_expert
        score = jnp.where(hit_column, row_order, 0).astype(jnp.int32)
        _, chosen = lax.top_k(score, pick_count)
        row_inputs = normed[chosen]
        gate_value = jnp.dot(row_inputs, w_gate, preferred_element_type=jnp.float32)
        up_value = jnp.dot(row_inputs, w_up, preferred_element_type=jnp.float32)
        inner_value = (jax.nn.silu(gate_value) * up_value).astype(jnp.bfloat16)
        result = jnp.dot(inner_value, w_down, preferred_element_type=jnp.float32)
        return (accumulated.at[chosen].add(mix_column[chosen][:, None] * result), None)
    start_value = jnp.zeros((row_count, hidden.shape[1]), jnp.float32)
    routed, _ = lax.scan(one_expert, start_value, (hit_any.T, by_expert.T, gate_proj, up_proj, down_proj))
    shared_inner = (jax.nn.silu(jnp.dot(normed, shared_gate, preferred_element_type=jnp.float32)) * jnp.dot(normed, shared_up, preferred_element_type=jnp.float32)).astype(jnp.bfloat16)
    shared = jnp.dot(shared_inner, shared_down, preferred_element_type=jnp.float32)
    return jnp.where(is_live[:, None], routed + shared, 0.0).astype(jnp.bfloat16)
```

```python
import functools

import jax
import jax.numpy as jnp
from jax import lax
from jax.experimental import pallas as pl
from jax.experimental.pallas import tpu as pltpu
from jax.sharding import PartitionSpec as P

epsilon = 1e-06
MESH = pl.DeviceIdType.MESH
F32 = jnp.float32
BF16 = jnp.bfloat16


def factors(ep, tp):
    x_size = 1
    while x_size * x_size * 4 <= ep and ep % (x_size * 2) == 0:
        x_size *= 2
    return x_size, ep // x_size, tp // 2


def kernel(
    ep, tp, hid, gain, wsend, wg_h, wu_h, wd_h, sg_h, su_h, sd_h, out,
    wg, wu, wd, sg, su, gath, xg, gains, wrecv, ss, acc_g, acc_u, sacc_g, sacc_u, inner,
    part, from_core, from_diag, from_x, from_y, from_z,
    local_sem, send_sem, gat_sem, sib_sem, gain_sem, w_sem, core_sem, diag_sem, x_sem, y_sem, z_sem,
):
    X, Z, Y = factors(ep, tp)
    S, Dt = hid.shape
    LE, D, F = wg.shape
    SF = sg.shape[1]
    R = ep * S
    ZS = Z * S
    half = Z // 2
    me_e, me_t = lax.axis_index("ep"), lax.axis_index("tp")
    z, x = me_e // X, me_e % X
    y, c = me_t // 2, me_t % 2

    def loc(dx=0, dy=0, dz=0, dc=0):
        return ((z + dz) % Z) * X + (x + dx) % X, ((y + dy) % Y) * 2 + (c + dc) % 2

    copies = []

    def load(src, dst):
        copy = pltpu.make_async_copy(src, dst, local_sem.at[len(copies)])
        copy.start()
        copies.append(copy)

    load(wg_h, wg)
    load(wu_h, wu)
    load(sg_h, sg)
    load(su_h, su)
    for e in range(LE):
        load(wd_h.at[e], wd.at[pl.ds(e * F, F)])
    load(sd_h, wd.at[pl.ds(LE * F, SF)])

    barrier = pltpu.get_barrier_semaphore()
    for de in range(1, ep):
        pl.semaphore_signal(barrier, inc=1, device_id=((me_e + de) % ep, me_t), device_id_type=MESH)
    for dt in range(1, tp):
        pl.semaphore_signal(barrier, inc=1, device_id=(me_e, (me_t + dt) % tp), device_id_type=MESH)
    pl.semaphore_wait(barrier, ep + tp - 2)

    sends = []

    def send(src, dst, rsem, device):
        copy = pltpu.make_async_remote_copy(
            src_ref=src, dst_ref=dst, send_sem=send_sem.at[len(sends)], recv_sem=rsem,
            device_id=device, device_id_type=MESH)
        copy.start()
        sends.append(copy)

    def arrived(dst, rsem):
        pltpu.make_async_remote_copy(
            src_ref=dst, dst_ref=dst, send_sem=send_sem.at[0], recv_sem=rsem,
            device_id=loc(dc=1), device_id_type=MESH).wait_recv()

    def row_of(xx, zz):
        return pl.multiple_of((xx * Z + zz) * S, S)

    def block(dx, dy, dz, dc=0):
        t = ((y - dy + Y) % Y) * 2 + (c + dc) % 2
        return gath.at[t, pl.ds(row_of((x - dx + X) % X, (z - dz + Z) % Z), S)]

    def slot(dx, dy, dz):
        return (dx * Y + dy) * Z + dz

    def pass_on(dx, dy, dz):
        own = dx == 0 and dy == 0 and dz == 0
        here = block(dx, dy, dz)
        if own:
            src = hid
        else:
            arrived(here, gat_sem.at[slot(dx, dy, dz)])
            src = here
        if own:
            for k in sorted(range(1, Z), key=lambda k: min(k, Z - k)):
                send(src, here, gat_sem.at[slot(0, 0, k)], loc(dz=k))
        if dx == 0 and (dy == 0 or dz >= half):
            for k in range(1, X):
                send(src, here, gat_sem.at[slot(k, dy, dz)], loc(dx=k))
        if dy == 0 and (dx == 0 or dz < half):
            for k in range(1, Y):
                send(src, here, gat_sem.at[slot(dx, k, dz)], loc(dy=k))
        send(src, here, sib_sem.at[slot(dx, dy, dz)], loc(dc=1))

    pass_on(0, 0, 0)
    for dt in range(1, tp):
        send(gain, gains.at[me_t], gain_sem.at[dt], (me_e, (me_t + dt) % tp))
    for de in range(1, ep):
        to = (me_e + de) % ep
        send(wsend.at[to], wrecv.at[me_e], w_sem.at[de], (to, me_t))
    gath[me_t, pl.ds(row_of(x, z), S)] = hid[...]
    gains[me_t] = gain[...]
    wrecv[me_e] = wsend[me_e]
    inner[:, LE * F:] = jnp.zeros((R, SF), BF16)
    ss[...] = jnp.zeros_like(ss)

    def line(dz):
        for dx in range(1, X):
            pass_on(dx, 0, dz)
        for dy in range(1, Y):
            pass_on(0, dy, dz)

    previous = 0
    for dz in sorted(range(1, Z), key=lambda k: min(k, Z - k)):
        pass_on(0, 0, dz)
        line(previous)
        previous = dz
    line(previous)
    for dt in range(1, tp):
        arrived(gains.at[(me_t + tp - dt) % tp], gain_sem.at[dt])
    waited = [False]

    rows_tile = min(R, 256)

    def project(dy, dc, first):
        t = ((y - dy + Y) % Y) * 2 + (c + dc) % 2

        def scale_rows(i, carry):
            rows = pl.ds(pl.multiple_of(i * S, S), S)
            values = gath[t, rows, :].astype(F32)
            squares = values * values
            total = squares[:, :128]
            for k in range(1, Dt // 128):
                total += squares[:, k * 128:(k + 1) * 128]
            ss[rows, :] += total
            xg[rows, :] = (values * gains[t]).astype(BF16)
            return carry

        lax.fori_loop(0, ep, scale_rows, 0)
        if not waited[0]:
            for k in range(4):
                copies[k].wait()
            waited[0] = True
        depth = pl.ds(pl.multiple_of(t * Dt, Dt), Dt)

        def experts(i, carry):
            e = i // (R // rows_tile)
            rows = pl.ds(pl.multiple_of((i % (R // rows_tile)) * rows_tile, rows_tile), rows_tile)
            g = jnp.dot(xg[rows, :], wg[e, depth, :], preferred_element_type=F32)
            u = jnp.dot(xg[rows, :], wu[e, depth, :], preferred_element_type=F32)
            if first:
                acc_g[e, rows, :] = g
                acc_u[e, rows, :] = u
            else:
                acc_g[e, rows, :] += g
                acc_u[e, rows, :] += u
            return carry

        lax.fori_loop(0, LE * (R // rows_tile), experts, 0)
        mine = xg[pl.ds(row_of(x, z), S), :]
        g = jnp.dot(mine, sg[depth, :], preferred_element_type=F32)
        u = jnp.dot(mine, su[depth, :], preferred_element_type=F32)
        if first:
            sacc_g[...] = g
            sacc_u[...] = u
        else:
            sacc_g[...] += g
            sacc_u[...] += u

    def from_sibling(dy):
        for dx in range(X):
            for dz in range(Z):
                arrived(block(dx, dy, dz, 1), sib_sem.at[slot(dx, dy, dz)])

    project(0, 0, True)
    for dz in range(Z):
        for dx in range(1, X):
            for dy in range(1, Y):
                pass_on(dx, dy, dz)
    from_sibling(0)
    project(0, 1, False)
    for dy in range(1, Y):
        project(dy, 0, False)
        from_sibling(dy)
        project(dy, 1, False)

    for de in range(1, ep):
        arrived(wrecv.at[(me_e + ep - de) % ep], w_sem.at[de])

    def scale_of(rows):
        return lax.rsqrt(jnp.sum(ss[rows, :], axis=1, keepdims=True) / D + epsilon)

    def gated(g, u):
        return g / (1.0 + jnp.exp(-g)) * u

    lanes = lax.broadcasted_iota(jnp.int32, (S, 128), 1)
    diagonal = lanes == lax.broadcasted_iota(jnp.int32, (S, 128), 0)

    def finish(i, carry):
        rows = pl.ds(pl.multiple_of(i * S, S), S)
        scale = scale_of(rows)
        weights = wrecv[(i % Z) * X + i // Z]
        for e in range(LE):
            column = jnp.sum(jnp.where(diagonal, weights[e:e + 1, :], 0.0), axis=1, keepdims=True)
            value = gated(acc_g[e, rows, :] * scale, acc_u[e, rows, :] * scale) * column
            inner[rows, e * F:(e + 1) * F] = value.astype(BF16)
        return carry

    lax.fori_loop(0, ep, finish, 0)
    own_rows = pl.ds(row_of(x, z), S)
    own_scale = scale_of(own_rows)
    inner[own_rows, LE * F:] = gated(sacc_g[...] * own_scale, sacc_u[...] * own_scale).astype(BF16)
    for copy in copies[4:]:
        copy.wait()

    tile = min(Dt, 256)

    def down(dx, dy, dc):
        rows = pl.ds(pl.multiple_of(((x + dx) % X) * ZS, ZS), ZS)
        t = ((y + dy) % Y) * 2 + (c + dc) % 2
        K = LE * F + (SF if dx == 0 else 0)

        def columns(n, carry):
            cols = pl.ds(pl.multiple_of(n * tile, tile), tile)
            wide = pl.ds(pl.multiple_of(t * Dt + n * tile, tile), tile)
            value = jnp.dot(inner[rows, :K], wd[:K, wide], preferred_element_type=F32)
            part[t, rows, cols] = value.astype(BF16)
            return carry

        lax.fori_loop(0, Dt // tile, columns, 0)

    def t_of(dy, dc=0):
        return ((y + dy) % Y) * 2 + (c + dc) % 2

    def line_rows(dx):
        return pl.ds(pl.multiple_of(((x + dx) % X) * ZS, ZS), ZS)

    def start_chunk(dx, dy):
        down(dx, dy, 1)
        send(part.at[t_of(dy, 1), line_rows(dx)], from_core.at[dx, dy], core_sem.at[dx * Y + dy], loc(dc=1))
        down(dx, dy, 0)

    def reduce_chunk(dx, dy):
        arrived(from_core.at[dx, dy], core_sem.at[dx * Y + dy])
        order = list(range(Z))
        for k in order:
            zz = k if dx or dy else (z + (k + 1)) % Z
            rows = pl.ds(row_of((x + dx) % X, zz), S)
            core_rows = pl.ds(pl.multiple_of(zz * S, S), S)
            total = part[t_of(dy), rows, :].astype(F32) + from_core[dx, dy, core_rows, :].astype(F32)
            if dx and not dy and k < half:
                for b in range(1, Y):
                    arrived(from_diag.at[dx - 1, b - 1, k], diag_sem.at[((dx - 1) * (Y - 1) + b - 1) * Z + k])
                    total += from_diag[dx - 1, b - 1, k].astype(F32)
            if dy and not dx and k >= half:
                for a in range(1, X):
                    arrived(from_diag.at[a - 1, dy - 1, k], diag_sem.at[((a - 1) * (Y - 1) + dy - 1) * Z + k])
                    total += from_diag[a - 1, dy - 1, k].astype(F32)
            if not dx and not dy:
                if k == 0:
                    for zk in range(Z):
                        for a in range(1, X):
                            arrived(from_x.at[a - 1, zk], x_sem.at[(a - 1) * Z + zk])
                        for b in range(1, Y):
                            arrived(from_y.at[b - 1, zk], y_sem.at[(b - 1) * Z + zk])
                for a in range(1, X):
                    total += from_x[a - 1, zz].astype(F32)
                for b in range(1, Y):
                    total += from_y[b - 1, zz].astype(F32)
                if k == Z - 1:
                    for dz in range(1, Z):
                        arrived(from_z.at[dz - 1], z_sem.at[dz])
                        total += from_z[dz - 1].astype(F32)
                    out[...] = total.astype(BF16)
                    return
            part[t_of(dy), rows, :] = total.astype(BF16)
            src = part.at[t_of(dy), rows]
            if dx and dy:
                sem = diag_sem.at[((dx - 1) * (Y - 1) + dy - 1) * Z + k]
                send(src, from_diag.at[dx - 1, dy - 1, k], sem, loc(dy=dy) if k < half else loc(dx=dx))
            elif dx:
                send(src, from_x.at[dx - 1, k], x_sem.at[(dx - 1) * Z + k], loc(dx=dx))
            elif dy:
                send(src, from_y.at[dy - 1, k], y_sem.at[(dy - 1) * Z + k], loc(dy=dy))
            else:
                send(src, from_z.at[k], z_sem.at[k + 1], loc(dz=k + 1))

    chunks = [(dx, dy) for dx in range(X) for dy in range(Y)]
    chunks.sort(key=lambda p: -((p[0] > 0) + (p[1] > 0)))
    start_chunk(*chunks[0])
    for before, after in zip(chunks, chunks[1:]):
        start_chunk(*after)
        reduce_chunk(*before)
    reduce_chunk(*chunks[-1])
    for copy in sends:
        copy.wait_send()


def solution(mesh):
    ep, tp = mesh.shape["ep"], mesh.shape["tp"]
    X, Z, Y = factors(ep, tp)

    def body(hidden, norm_gain, expert_ids, route_weights, lengths, gate_proj, up_proj, down_proj,
             shared_gate, shared_up, shared_down):
        S, Dt = hidden.shape
        LE, D, F = gate_proj.shape
        SF = shared_gate.shape[1]
        R = ep * S
        span = S // lengths.shape[0]
        offsets = jnp.arange(S, dtype=jnp.int32) % span
        is_live = offsets < jnp.repeat(lengths, span)
        mixing = jnp.where(is_live[:, None], route_weights, 0.0)
        padded = -(-LE // 8) * 8
        named = jnp.arange(padded, dtype=jnp.int32)[None, :] + LE * jnp.arange(ep, dtype=jnp.int32)[:, None]
        hit = expert_ids.T[:, None, None, :] == named[None, :, :, None]
        wsend = jnp.sum(jnp.where(hit, mixing.T[:, None, None, :], 0.0), axis=0)
        wsend = jnp.pad(wsend, ((0, 0), (0, 0), (0, 128 - S)))
        blocks = X * Y * Z
        n_sends = 2 * blocks - 1 + tp - 1 + ep - 1 + X * Y + blocks - 1
        vmem = pl.BlockSpec(memory_space=pltpu.VMEM)
        hbm = pl.BlockSpec(memory_space=pl.ANY)
        dma = pltpu.SemaphoreType.DMA
        combined = pl.pallas_call(
            functools.partial(kernel, ep, tp),
            out_shape=jax.ShapeDtypeStruct((S, Dt), BF16),
            in_specs=[vmem] * 3 + [hbm] * 6,
            out_specs=vmem,
            scratch_shapes=[
                pltpu.VMEM((LE, D, F), BF16),
                pltpu.VMEM((LE, D, F), BF16),
                pltpu.VMEM((LE * F + SF, D), BF16),
                pltpu.VMEM((D, SF), BF16),
                pltpu.VMEM((D, SF), BF16),
                pltpu.VMEM((tp, R, Dt), BF16),
                pltpu.VMEM((R, Dt), BF16),
                pltpu.VMEM((tp, 1, Dt), F32),
                pltpu.VMEM((ep, padded, 128), F32),
                pltpu.VMEM((R, 128), F32),
                pltpu.VMEM((LE, R, F), F32),
                pltpu.VMEM((LE, R, F), F32),
                pltpu.VMEM((S, SF), F32),
                pltpu.VMEM((S, SF), F32),
                pltpu.VMEM((R, LE * F + SF), BF16),
                pltpu.VMEM((tp, R, Dt), BF16),
                pltpu.VMEM((X, Y, Z * S, Dt), BF16),
                pltpu.VMEM((max(X - 1, 1), max(Y - 1, 1), Z, S, Dt), BF16),
                pltpu.VMEM((max(X - 1, 1), Z, S, Dt), BF16),
                pltpu.VMEM((max(Y - 1, 1), Z, S, Dt), BF16),
                pltpu.VMEM((max(Z - 1, 1), S, Dt), BF16),
                dma((5 + LE,)),
                dma((n_sends,)),
                dma((blocks,)),
                dma((blocks,)),
                dma((tp,)),
                dma((ep,)),
                dma((X * Y,)),
                dma((max((X - 1) * (Y - 1) * Z, 1),)),
                dma((max((X - 1) * Z, 1),)),
                dma((max((Y - 1) * Z, 1),)),
                dma((Z,)),
            ],
            compiler_params=pltpu.CompilerParams(
                collective_id=0, has_side_effects=True, vmem_limit_bytes=60 * 1024 * 1024),
        )(hidden, norm_gain[None, :], wsend, gate_proj, up_proj, down_proj, shared_gate, shared_up, shared_down)
        return jnp.where(is_live[:, None], combined, jnp.zeros_like(combined))

    placed = (
        P("ep", "tp"),
        P("tp"),
        P("ep", None),
        P("ep", None),
        P("ep"),
        P("ep", None, "tp"),
        P("ep", None, "tp"),
        P("ep", "tp", None),
        P(None, "tp"),
        P(None, "tp"),
        P("tp", None),
    )
    return jax.shard_map(body, mesh=mesh, in_specs=placed, out_specs=P("ep", "tp"), check_vma=False)
```

```python
import functools

import jax
import jax.numpy as jnp
from jax import lax
from jax.experimental import pallas as pl
from jax.experimental.pallas import tpu as pltpu
from jax.sharding import PartitionSpec as P

epsilon = 1e-06
MESH = pl.DeviceIdType.MESH
F32 = jnp.float32
BF16 = jnp.bfloat16


def factors(ep, tp):
    x_size = 1
    while x_size * x_size * 4 <= ep and ep % (x_size * 2) == 0:
        x_size *= 2
    return x_size, ep // x_size, tp // 2


def kernel(
    ep, tp, hid, gain, ids, mix, lengths, wg_h, wu_h, wd_h, sg_h, su_h, sd_h, out,
    wg, wu, wd, sg, su, gath, xg, gains, wsend, wrecv, ss, acc_g, acc_u, sacc_g, sacc_u, inner,
    part, from_core, from_diag, from_x, from_y, from_z,
    local_sem, send_sem, gat_sem, sib_sem, gain_sem, w_sem, core_sem, diag_sem, x_sem, y_sem, z_sem,
):
    X, Z, Y = factors(ep, tp)
    S, Dt = hid.shape
    LE, D, F = wg.shape
    SF = sg.shape[1]
    R = ep * S
    ZS = Z * S
    near = sorted(range(1, Z), key=lambda k: min(k, Z - k))
    first_x = [k for p, k in enumerate([0] + near) if p % 2 == 0]
    me_e, me_t = lax.axis_index("ep"), lax.axis_index("tp")
    z, x = me_e // X, me_e % X
    y, c = me_t // 2, me_t % 2

    def loc(dx=0, dy=0, dz=0, dc=0):
        return ((z + dz) % Z) * X + (x + dx) % X, ((y + dy) % Y) * 2 + (c + dc) % 2

    copies = []

    def load(src, dst):
        copy = pltpu.make_async_copy(src, dst, local_sem.at[len(copies)])
        copy.start()
        copies.append(copy)

    load(wg_h, wg)
    load(wu_h, wu)
    load(sg_h, sg)
    load(su_h, su)
    for e in range(LE):
        load(wd_h.at[e], wd.at[pl.ds(e * F, F)])
    load(sd_h, wd.at[pl.ds(LE * F, SF)])

    barrier = pltpu.get_barrier_semaphore()
    for de in range(1, ep):
        pl.semaphore_signal(barrier, inc=1, device_id=((me_e + de) % ep, me_t), device_id_type=MESH)
    for dt in range(1, tp):
        pl.semaphore_signal(barrier, inc=1, device_id=(me_e, (me_t + dt) % tp), device_id_type=MESH)
    pl.semaphore_wait(barrier, ep + tp - 2)

    sends = []

    def send(src, dst, rsem, device):
        copy = pltpu.make_async_remote_copy(
            src_ref=src, dst_ref=dst, send_sem=send_sem.at[len(sends)], recv_sem=rsem,
            device_id=device, device_id_type=MESH)
        copy.start()
        sends.append(copy)

    def arrived(dst, rsem):
        pltpu.make_async_remote_copy(
            src_ref=dst, dst_ref=dst, send_sem=send_sem.at[0], recv_sem=rsem,
            device_id=loc(dc=1), device_id_type=MESH).wait_recv()

    def row_of(xx, zz):
        return pl.multiple_of((xx * Z + zz) * S, S)

    def block(dx, dy, dz, dc=0):
        t = ((y - dy + Y) % Y) * 2 + (c + dc) % 2
        return gath.at[t, pl.ds(row_of((x - dx + X) % X, (z - dz + Z) % Z), S)]

    def slot(dx, dy, dz):
        return (dx * Y + dy) * Z + dz

    def pass_on(dx, dy, dz):
        own = dx == 0 and dy == 0 and dz == 0
        here = block(dx, dy, dz)
        if own:
            src = hid
        else:
            arrived(here, gat_sem.at[slot(dx, dy, dz)])
            src = here
        if own:
            for k in near:
                send(src, here, gat_sem.at[slot(0, 0, k)], loc(dz=k))
        if dx == 0 and (dy == 0 or dz not in first_x):
            for k in range(1, X):
                send(src, here, gat_sem.at[slot(k, dy, dz)], loc(dx=k))
        if dy == 0 and (dx == 0 or dz in first_x):
            for k in range(1, Y):
                send(src, here, gat_sem.at[slot(dx, k, dz)], loc(dy=k))
        send(src, here, sib_sem.at[slot(dx, dy, dz)], loc(dc=1))

    pass_on(0, 0, 0)
    for dt in range(1, tp):
        send(gain, gains.at[me_t], gain_sem.at[dt], (me_e, (me_t + dt) % tp))
    span = S // lengths.shape[0]
    position = lax.broadcasted_iota(jnp.int32, (1, S), 1)
    limit = jnp.zeros((1, S), jnp.int32)
    for q in range(lengths.shape[0]):
        limit = jnp.where(position // span == q, lengths[q], limit)
    mixing = jnp.where(position % span < limit, mix[...], 0.0)
    named = ids[...]
    wsend[...] = jnp.zeros_like(wsend)

    def weights_for(j, carry):
        for e in range(LE):
            hit = named == j * LE + e
            wsend[j, e:e + 1, :S] = jnp.sum(jnp.where(hit, mixing, 0.0), axis=0, keepdims=True)
        return carry

    lax.fori_loop(0, ep, weights_for, 0)
    for de in range(1, ep):
        to = (me_e + de) % ep
        send(wsend.at[to], wrecv.at[me_e], w_sem.at[de], (to, me_t))
    gath[me_t, pl.ds(row_of(x, z), S)] = hid[...]
    gains[me_t] = gain[...]
    wrecv[me_e] = wsend[me_e]
    inner[:, LE * F:] = jnp.zeros((R, SF), BF16)
    ss[...] = jnp.zeros_like(ss)

    def line(dz):
        for dx in range(1, X):
            pass_on(dx, 0, dz)
        for dy in range(1, Y):
            pass_on(0, dy, dz)

    previous = 0
    for dz in near:
        pass_on(0, 0, dz)
        line(previous)
        previous = dz
    line(previous)
    for dt in range(1, tp):
        arrived(gains.at[(me_t + tp - dt) % tp], gain_sem.at[dt])
    waited = [False]

    rows_tile = min(R, 256)

    def project(dy, dc, first):
        t = ((y - dy + Y) % Y) * 2 + (c + dc) % 2

        def scale_rows(i, carry):
            rows = pl.ds(pl.multiple_of(i * S, S), S)
            values = gath[t, rows, :].astype(F32)
            squares = values * values
            total = squares[:, :128]
            for k in range(1, Dt // 128):
                total += squares[:, k * 128:(k + 1) * 128]
            ss[rows, :] += total
            xg[rows, :] = (values * gains[t]).astype(BF16)
            return carry

        lax.fori_loop(0, ep, scale_rows, 0)
        if not waited[0]:
            for k in range(4):
                copies[k].wait()
            waited[0] = True
        depth = pl.ds(pl.multiple_of(t * Dt, Dt), Dt)

        def experts(i, carry):
            e = i // (R // rows_tile)
            rows = pl.ds(pl.multiple_of((i % (R // rows_tile)) * rows_tile, rows_tile), rows_tile)
            g = jnp.dot(xg[rows, :], wg[e, depth, :], preferred_element_type=F32)
            u = jnp.dot(xg[rows, :], wu[e, depth, :], preferred_element_type=F32)
            if first:
                acc_g[e, rows, :] = g
                acc_u[e, rows, :] = u
            else:
                acc_g[e, rows, :] += g
                acc_u[e, rows, :] += u
            return carry

        lax.fori_loop(0, LE * (R // rows_tile), experts, 0)
        mine = xg[pl.ds(row_of(x, z), S), :]
        g = jnp.dot(mine, sg[depth, :], preferred_element_type=F32)
        u = jnp.dot(mine, su[depth, :], preferred_element_type=F32)
        if first:
            sacc_g[...] = g
            sacc_u[...] = u
        else:
            sacc_g[...] += g
            sacc_u[...] += u

    def from_sibling(dy):
        for dx in range(X):
            for dz in range(Z):
                arrived(block(dx, dy, dz, 1), sib_sem.at[slot(dx, dy, dz)])

    project(0, 0, True)
    for dz in [0] + near:
        for dx in range(1, X):
            for dy in range(1, Y):
                pass_on(dx, dy, dz)
    from_sibling(0)
    project(0, 1, False)
    for dy in range(1, Y):
        project(dy, 0, False)
        from_sibling(dy)
        project(dy, 1, False)

    for de in range(1, ep):
        arrived(wrecv.at[(me_e + ep - de) % ep], w_sem.at[de])

    def scale_of(rows):
        return lax.rsqrt(jnp.sum(ss[rows, :], axis=1, keepdims=True) / D + epsilon)

    def gated(g, u):
        return g / (1.0 + jnp.exp(-g)) * u

    lanes = lax.broadcasted_iota(jnp.int32, (S, 128), 1)
    diagonal = lanes == lax.broadcasted_iota(jnp.int32, (S, 128), 0)

    def finish(i, carry):
        rows = pl.ds(pl.multiple_of(i * S, S), S)
        scale = scale_of(rows)
        weights = wrecv[(i % Z) * X + i // Z]
        for e in range(LE):
            column = jnp.sum(jnp.where(diagonal, weights[e:e + 1, :], 0.0), axis=1, keepdims=True)
            value = gated(acc_g[e, rows, :] * scale, acc_u[e, rows, :] * scale) * column
            inner[rows, e * F:(e + 1) * F] = value.astype(BF16)
        return carry

    lax.fori_loop(0, ep, finish, 0)
    own_rows = pl.ds(row_of(x, z), S)
    own_scale = scale_of(own_rows)
    inner[own_rows, LE * F:] = gated(sacc_g[...] * own_scale, sacc_u[...] * own_scale).astype(BF16)
    for copy in copies[4:]:
        copy.wait()

    tile = min(Dt, 512)

    def down(dx, dy, dc):
        rows = pl.ds(pl.multiple_of(((x + dx) % X) * ZS, ZS), ZS)
        t = ((y + dy) % Y) * 2 + (c + dc) % 2
        K = LE * F + (SF if dx == 0 else 0)

        def columns(n, carry):
            cols = pl.ds(pl.multiple_of(n * tile, tile), tile)
            wide = pl.ds(pl.multiple_of(t * Dt + n * tile, tile), tile)
            value = jnp.dot(inner[rows, :K], wd[:K, wide], preferred_element_type=F32)
            part[t, rows, cols] = value.astype(BF16)
            return carry

        lax.fori_loop(0, Dt // tile, columns, 0)

    def t_of(dy, dc=0):
        return ((y + dy) % Y) * 2 + (c + dc) % 2

    def line_rows(dx):
        return pl.ds(pl.multiple_of(((x + dx) % X) * ZS, ZS), ZS)

    def start_chunk(dx, dy):
        down(dx, dy, 1)
        send(part.at[t_of(dy, 1), line_rows(dx)], from_core.at[dx, dy], core_sem.at[dx * Y + dy], loc(dc=1))
        down(dx, dy, 0)

    order = near + [0]

    def diag_slot(dx, dy, p):
        return ((dx - 1) * (Y - 1) + dy - 1) * Z + p

    def reduce_block(dx, dy, p):
        zz = (z + order[p]) % Z
        rows = pl.ds(row_of((x + dx) % X, zz), S)
        core_rows = pl.ds(pl.multiple_of(zz * S, S), S)
        total = part[t_of(dy), rows, :].astype(F32) + from_core[dx, dy, core_rows, :].astype(F32)
        if dx and not dy and p % 2 == 1:
            for b in range(1, Y):
                arrived(from_diag.at[dx - 1, b - 1, p], diag_sem.at[diag_slot(dx, b, p)])
                total += from_diag[dx - 1, b - 1, p].astype(F32)
        if dy and not dx and p % 2 == 0:
            for a in range(1, X):
                arrived(from_diag.at[a - 1, dy - 1, p], diag_sem.at[diag_slot(a, dy, p)])
                total += from_diag[a - 1, dy - 1, p].astype(F32)
        if not dx and not dy:
            for a in range(1, X):
                arrived(from_x.at[a - 1, p], x_sem.at[(a - 1) * Z + p])
                total += from_x[a - 1, p].astype(F32)
            for b in range(1, Y):
                arrived(from_y.at[b - 1, p], y_sem.at[(b - 1) * Z + p])
                total += from_y[b - 1, p].astype(F32)
            if p == Z - 1:
                for dz in near:
                    arrived(from_z.at[dz - 1], z_sem.at[dz])
                    total += from_z[dz - 1].astype(F32)
                out[...] = total.astype(BF16)
                return
        part[t_of(dy), rows, :] = total.astype(BF16)
        src = part.at[t_of(dy), rows]
        if dx and dy:
            sem = diag_sem.at[diag_slot(dx, dy, p)]
            send(src, from_diag.at[dx - 1, dy - 1, p], sem, loc(dx=dx) if p % 2 == 0 else loc(dy=dy))
        elif dx:
            send(src, from_x.at[dx - 1, p], x_sem.at[(dx - 1) * Z + p], loc(dx=dx))
        elif dy:
            send(src, from_y.at[dy - 1, p], y_sem.at[(dy - 1) * Z + p], loc(dy=dy))
        else:
            dz = order[p]
            send(src, from_z.at[dz - 1], z_sem.at[dz], loc(dz=dz))

    def core_arrived(dx, dy):
        arrived(from_core.at[dx, dy], core_sem.at[dx * Y + dy])

    far = [(dx, dy) for dx in range(1, X) for dy in range(1, Y)]
    sides_x = [(dx, 0) for dx in range(1, X)]
    sides_y = [(0, dy) for dy in range(1, Y)]
    for pair in far:
        start_chunk(*pair)
    for pair in sides_x:
        start_chunk(*pair)
    for pair in far:
        core_arrived(*pair)
    for p in range(Z):
        for pair in far:
            reduce_block(*pair, p)
    for pair in sides_y:
        start_chunk(*pair)
    for pair in sides_x + sides_y:
        core_arrived(*pair)
    y_order = list(range(Z))
    for p in range(0, Z - 1, 2):
        y_order[p], y_order[p + 1] = p + 1, p
    for i in range(Z):
        for pair in sides_x:
            reduce_block(*pair, i)
        for pair in sides_y:
            reduce_block(*pair, y_order[i])
        if i == 0:
            start_chunk(0, 0)
    core_arrived(0, 0)
    for p in range(Z):
        reduce_block(0, 0, p)
    for copy in sends:
        copy.wait_send()


def solution(mesh):
    ep, tp = mesh.shape["ep"], mesh.shape["tp"]
    X, Z, Y = factors(ep, tp)

    def body(hidden, norm_gain, expert_ids, route_weights, lengths, gate_proj, up_proj, down_proj,
             shared_gate, shared_up, shared_down):
        S, Dt = hidden.shape
        LE, D, F = gate_proj.shape
        SF = shared_gate.shape[1]
        R = ep * S
        span = S // lengths.shape[0]
        offsets = jnp.arange(S, dtype=jnp.int32) % span
        is_live = offsets < jnp.repeat(lengths, span)
        padded = -(-LE // 8) * 8
        blocks = X * Y * Z
        n_sends = 2 * blocks - 1 + tp - 1 + ep - 1 + X * Y + blocks - 1
        vmem = pl.BlockSpec(memory_space=pltpu.VMEM)
        hbm = pl.BlockSpec(memory_space=pl.ANY)
        dma = pltpu.SemaphoreType.DMA
        combined = pl.pallas_call(
            functools.partial(kernel, ep, tp),
            out_shape=jax.ShapeDtypeStruct((S, Dt), BF16),
            in_specs=[vmem] * 4 + [pl.BlockSpec(memory_space=pltpu.SMEM)] + [hbm] * 6,
            out_specs=vmem,
            scratch_shapes=[
                pltpu.VMEM((LE, D, F), BF16),
                pltpu.VMEM((LE, D, F), BF16),
                pltpu.VMEM((LE * F + SF, D), BF16),
                pltpu.VMEM((D, SF), BF16),
                pltpu.VMEM((D, SF), BF16),
                pltpu.VMEM((tp, R, Dt), BF16),
                pltpu.VMEM((R, Dt), BF16),
                pltpu.VMEM((tp, 1, Dt), F32),
                pltpu.VMEM((ep, padded, 128), F32),
                pltpu.VMEM((ep, padded, 128), F32),
                pltpu.VMEM((R, 128), F32),
                pltpu.VMEM((LE, R, F), F32),
                pltpu.VMEM((LE, R, F), F32),
                pltpu.VMEM((S, SF), F32),
                pltpu.VMEM((S, SF), F32),
                pltpu.VMEM((R, LE * F + SF), BF16),
                pltpu.VMEM((tp, R, Dt), BF16),
                pltpu.VMEM((X, Y, Z * S, Dt), BF16),
                pltpu.VMEM((max(X - 1, 1), max(Y - 1, 1), Z, S, Dt), BF16),
                pltpu.VMEM((max(X - 1, 1), Z, S, Dt), BF16),
                pltpu.VMEM((max(Y - 1, 1), Z, S, Dt), BF16),
                pltpu.VMEM((max(Z - 1, 1), S, Dt), BF16),
                dma((5 + LE,)),
                dma((n_sends,)),
                dma((blocks,)),
                dma((blocks,)),
                dma((tp,)),
                dma((ep,)),
                dma((X * Y,)),
                dma((max((X - 1) * (Y - 1) * Z, 1),)),
                dma((max((X - 1) * Z, 1),)),
                dma((max((Y - 1) * Z, 1),)),
                dma((Z,)),
            ],
            compiler_params=pltpu.CompilerParams(
                collective_id=0, has_side_effects=True, vmem_limit_bytes=60 * 1024 * 1024),
        )(hidden, norm_gain[None, :], expert_ids.T, route_weights.T, lengths, gate_proj, up_proj, down_proj,
          shared_gate, shared_up, shared_down)
        return jnp.where(is_live[:, None], combined, jnp.zeros_like(combined))

    placed = (
        P("ep", "tp"),
        P("tp"),
        P("ep", None),
        P("ep", None),
        P("ep"),
        P("ep", None, "tp"),
        P("ep", None, "tp"),
        P("ep", "tp", None),
        P(None, "tp"),
        P(None, "tp"),
        P("tp", None),
    )
    return jax.shard_map(body, mesh=mesh, in_specs=placed, out_specs=P("ep", "tp"), check_vma=False)
```
